256 devices in a mesh: sp: 64 (over z, x, core), tp: 4 (over y).
Axes of the slice: x: 4, y: 4, z: 8, core: 2. Of those that a mesh axis runs over, the one named last changes fastest.
Arguments:
- residual: bfloat16 [8192, 2048], P(('sp', 'tp')), may hold values from -6 to 6
- query_rows: bfloat16 [8192, 1024], P('sp', 'tp'), may hold values from -6 to 6
- key_rows: bfloat16 [8192, 512], P('sp', 'tp'), may hold values from -6 to 6
- value_rows: bfloat16 [8192, 512], P('sp', 'tp'), may hold values from -8 to 8
- head_offset: float32 [8], P('tp'), may hold values from -13 to -3
- w_out: bfloat16 [1024, 2048], P('tp'), may hold values from -0.5 to 0.5
- norm_gain: float32 [2, 2048], replicated, may hold values from 0.1 to 1.9
- norm_bias: float32 [2, 2048], replicated, may hold values from -1.5 to 1.5
- routing: int32 [8192, 2], P(('sp', 'tp')), may hold values from 0 to 63, all different within a row; in each aligned block of 32 rows (0 to 31, 32 to 63, ...) at most 2 rows name the same one
- route_weight: float32 [8192, 2], P(('sp', 'tp')), may hold values from 0.2 to 1
- w_exp_gate: bfloat16 [64, 2048, 1024], P('sp', None, 'tp'), may hold values from -0.125 to 0.125
- w_exp_up: bfloat16 [64, 2048, 1024], P('sp', None, 'tp'), may hold values from -0.125 to 0.125
- w_exp_down: bfloat16 [64, 1024, 2048], P('sp', 'tp'), may hold values from -0.1875 to 0.1875
- w_shared_gate: bfloat16 [2048, 1024], P(None, 'tp'), may hold values from -0.125 to 0.125
- w_shared_up: bfloat16 [2048, 1024], P(None, 'tp'), may hold values from -0.125 to 0.125
- w_shared_down: bfloat16 [1024, 2048], P('tp'), may hold values from -0.1875 to 0.1875
Outputs:
- result: bfloat16 [8192, 2048], P(('sp', 'tp'))
The draws below stay inside these ranges and needn't reach their ends.
Inputs may be any that keep to these rules, and one draw needn't show every extreme that they name: `routing`: each row names 2 different experts; within the rows of one device (32 tokens) no expert is named by more than 2 of them, a bound that some block reaches.
All inputs are finite; a program needn't handle non-finite values.
Results may differ from the reference program's by a relative error of at most 0.013.
Values may be sent and summed in bfloat16 or wider, within the bound.
A program may use at most 64 MiB of HBM per device.

```python
import math
import jax
import jax.numpy as jnp
import numpy as np
from jax import lax

D = 2048
HEADS = 8
DH = 128
KV_HEADS = 4
EXPERT_FF = 1024
SHARED_FF = 1024
TOP_K = 2
TOK_DEV = 128
TOKENS = 8192
ROWS_DEV = 32
EXPERTS = 64
CAP = 2
N_TP = 4


def draw_value_rows(key, part):
    key_center = jax.random.fold_in(key, 11)
    key_noise = jax.random.fold_in(key, 12)
    center = jnp.clip(jax.random.normal(key_center, (1, KV_HEADS * DH), jnp.float32), -1.0, 1.0)
    noise = 2.0 * jnp.clip(jax.random.normal(key_noise, (TOKENS, KV_HEADS * DH), jnp.float32), -3.5, 3.5)
    return (center + noise).astype(jnp.bfloat16)


def draw_head_offset(key, part):
    key_pick = jax.random.fold_in(key, 21)
    key_slow = jax.random.fold_in(key, 22)
    key_fast = jax.random.fold_in(key, 23)
    keep_share = 0.5
    slow_heads = jax.random.uniform(key_pick, (HEADS,), jnp.float32) < keep_share
    slow_value = -jnp.log(0.6 * TOKENS) + jax.random.uniform(key_slow, (HEADS,), jnp.float32, -0.5, 0.5)
    fast_value = -jax.random.uniform(key_fast, (HEADS,), jnp.float32, 3.0, 4.5)
    return jnp.where(slow_heads, slow_value, fast_value).astype(jnp.float32)


def steps_of(rng, dims, cuts, smallest, high):
    def one(axis_at, blocks):
        draws = jax.random.uniform(jax.random.fold_in(jax.random.fold_in(rng, 6), axis_at), (blocks,), jnp.float32, smallest / len(cuts), high / len(cuts))
        return jnp.repeat(jnp.exp(draws), dims[axis_at] // blocks).reshape((-1,) + (1,) * (len(dims) - axis_at - 1))

    level = one(*cuts[0])
    for cut in cuts[1:]:
        level = level * one(*cut)
    return level


def routed_block(stream_key, own, number, rows, amount, top, reach, lean):
    sequence = jax.random.permutation(stream_key, amount)
    crowded, usual = shares(amount, rows * top, reach, lean, True), shares(amount, rows * top, reach, lean, False)
    places = jnp.arange(amount)

    def named(lengths, rotation):
        used = int((lengths > 0).sum())
        fixed = max(1, used // 4)
        moved = fixed + (places - fixed + rotation * (used - fixed)) % max(1, amount - fixed)
        return jnp.zeros((amount,), jnp.int32).at[sequence[jnp.where(places < fixed, places, moved)]].set(jnp.asarray(lengths, jnp.int32))

    lengths = jnp.where(number % 4 == 0, named(crowded, number // 4), named(usual, number - number // 4 - 1))
    mixed = jax.random.permutation(jax.random.fold_in(own, 3), amount)
    donor, sink = mixed[0:amount // 2 * 2:2], mixed[1:amount // 2 * 2:2]
    room = jnp.minimum(lengths[donor] - 1, reach - lengths[sink]) // 2
    room = jnp.where((donor == sequence[0]) | (sink == sequence[0]) | (lengths[sink] == 0), 0, jnp.maximum(room, 0))
    moved = jax.random.randint(jax.random.fold_in(own, 4), (amount // 2,), 0, 1 << 20) % (room + 1)
    lengths = lengths.at[donor].add(-moved).at[sink].add(moved)
    members = jnp.searchsorted(jnp.cumsum(lengths), jnp.arange(rows * top), side="right").astype(jnp.int32)
    listing = members.reshape(top, rows).T
    listing = listing[jax.random.permutation(jax.random.fold_in(own, 1), rows)]
    rotation = jax.random.randint(jax.random.fold_in(own, 2), (rows, 1), 0, top)
    return jnp.take_along_axis(listing, (jnp.arange(top)[None, :] + rotation) % top, axis=1)


def shares(amount, total, limit, skew, full):
    weights = [(1 << 20) // math.isqrt(standing ** skew) + 1 for standing in range(1, amount + 1)]
    largest = limit if full else min(limit, max(-(-total // amount), total * weights[0] // sum(weights)))
    least = 1 if total - largest >= amount - 1 else 0
    given, spare = [largest] + [least] * (amount - 1), total - largest - least * (amount - 1)
    while spare > 0:
        free = [i for i in range(1, amount) if given[i] < largest] or [i for i in range(1, amount) if given[i] < limit]
        pool, left = sum([weights[i] for i in free]), spare
        for i in free:
            more = min(limit - given[i], max(1, left * weights[i] // pool), spare)
            given[i] = given[i] + more
            spare = spare - more
    return np.array(given)


def centred(own_key, dims, deviation, reach, pieces=(), held_as=jnp.bfloat16):
    level = steps_of(own_key, dims, pieces, -0.22, 0.18) if pieces else 1.0
    array = jax.random.normal(own_key, dims, jnp.float32) * deviation * level
    return jnp.minimum(jnp.maximum(array, -reach), reach).astype(held_as)


def setup_inputs(seed: int = 0) -> dict:
    streams_of = jax.random.split(jax.random.key(seed), 17)
    residual = centred(streams_of[0], (TOKENS, D), 1.0, 6.0, ((0, 256),))
    query_rows = centred(streams_of[1], (TOKENS, HEADS * DH), 1.0, 6.0, ((0, 64), (1, 4)))
    key_rows = centred(streams_of[2], (TOKENS, KV_HEADS * DH), 1.0, 6.0, ((0, 64), (1, 4)))
    value_rows = draw_value_rows(jax.random.fold_in(streams_of[16], 71), 0)
    head_offset = draw_head_offset(jax.random.fold_in(streams_of[16], 71), 0)
    w_out = centred(streams_of[5], (HEADS * DH, D), (HEADS * DH // 8) ** -0.5, 0.5, ((0, 4),))
    norm_gain = jnp.clip(1.0 + 0.18 * jax.random.normal(streams_of[6], (2, D), jnp.float32), 0.1, 1.9)
    norm_bias = centred(streams_of[7], (2, D), 0.3, 1.5, (), jnp.float32)
    routing_keys = jax.random.split(jax.random.fold_in(streams_of[8], 1), TOKENS // ROWS_DEV)
    routing_turns = jax.random.permutation(jax.random.fold_in(streams_of[8], 3), TOKENS // ROWS_DEV)
    routing = jax.vmap(lambda own, number: routed_block(jax.random.fold_in(streams_of[8], 2), own, number, ROWS_DEV, EXPERTS, TOP_K, CAP, 1))(routing_keys, routing_turns).reshape((TOKENS, TOP_K))
    route_weight = jnp.clip(0.2 + 0.8 * jax.random.uniform(streams_of[9], (TOKENS, TOP_K), jnp.float32) ** steps_of(streams_of[9], (TOKENS, TOP_K), ((0, 256),), -0.2, 0.2), 0.2, 1.0)
    w_exp_gate = centred(streams_of[10], (EXPERTS, D, EXPERT_FF), D ** -0.5, 0.125, ((0, 64), (2, 4)))
    w_exp_up = centred(streams_of[11], (EXPERTS, D, EXPERT_FF), D ** -0.5, 0.125, ((0, 64), (2, 4)))
    w_exp_down = centred(streams_of[12], (EXPERTS, EXPERT_FF, D), EXPERT_FF ** -0.5, 0.1875, ((0, 64), (1, 4)))
    w_shared_gate = centred(streams_of[13], (D, SHARED_FF), D ** -0.5, 0.125, ((1, 4),))
    w_shared_up = centred(streams_of[14], (D, SHARED_FF), D ** -0.5, 0.125, ((1, 4),))
    w_shared_down = centred(streams_of[15], (SHARED_FF, D), SHARED_FF ** -0.5, 0.1875, ((0, 4),))
    return dict(residual=residual, query_rows=query_rows, key_rows=key_rows, value_rows=value_rows, head_offset=head_offset, w_out=w_out, norm_gain=norm_gain, norm_bias=norm_bias, routing=routing, route_weight=route_weight, w_exp_gate=w_exp_gate, w_exp_up=w_exp_up, w_exp_down=w_exp_down, w_shared_gate=w_shared_gate, w_shared_up=w_shared_up, w_shared_down=w_shared_down)


ALPHA = 8.0 ** 0.25
LN_EPS = 1e-05

def layer_norm(summed, gain, shift):
    center = summed - lax.optimization_barrier(jnp.mean(summed, axis=-1, keepdims=True))
    spread = lax.optimization_barrier(jnp.mean(center * center, axis=-1, keepdims=True))
    return (center * lax.rsqrt(spread + LN_EPS) * gain + shift).astype(jnp.bfloat16)

def split_down(hidden, down_weight, group_len):
    total = jnp.zeros((hidden.shape[0], down_weight.shape[1]), jnp.float32)
    for group_index in range(N_TP):
        lower = group_index * group_len
        part = jnp.dot(hidden[:, lower:lower + group_len], down_weight[lower:lower + group_len], preferred_element_type=jnp.float32)
        rounded = lax.optimization_barrier(part.astype(jnp.bfloat16))
        total = total + rounded.astype(jnp.float32)
    return total.astype(jnp.bfloat16)

def reference(residual, query_rows, key_rows, value_rows, head_offset, w_out, norm_gain, norm_bias, routing, route_weight, w_exp_gate, w_exp_up, w_exp_down, w_shared_gate, w_shared_up, w_shared_down):
    group_size = HEADS // KV_HEADS
    queries = query_rows.astype(jnp.float32).reshape(TOKENS, KV_HEADS, group_size, DH)
    keys_all = key_rows.astype(jnp.float32).reshape(TOKENS, KV_HEADS, DH)
    values_all = value_rows.astype(jnp.float32).reshape(TOKENS, KV_HEADS, DH)
    offset = head_offset.reshape(KV_HEADS, group_size)
    key_pos = jnp.arange(TOKENS, dtype=jnp.int32)

    def attend_block(first_row):
        block_queries = lax.dynamic_slice_in_dim(queries, first_row, TOK_DEV, 0)
        scores = jnp.einsum('tkgd,skd->kgts', block_queries, keys_all)
        scores = scores * DH ** (-0.5) + offset[:, :, None, None]
        query_pos = (first_row + jnp.arange(TOK_DEV, dtype=jnp.int32)).astype(jnp.int32)
        causal = key_pos[None, :] < query_pos[:, None]
        leftover = jnp.where(causal, jax.nn.log_sigmoid(-scores), 0.0)
        passed = lax.cumsum(leftover, axis=3, reverse=True) - leftover
        weights = jnp.where(causal, jnp.exp(jax.nn.log_sigmoid(scores) + passed), 0.0).astype(jnp.bfloat16)
        output = jnp.einsum('kgts,skd->tkgd', weights.astype(jnp.float32), values_all)
        return output.astype(jnp.bfloat16)
    starts = (jnp.arange(TOKENS // TOK_DEV, dtype=jnp.int32) * TOK_DEV).astype(jnp.int32)
    attended = lax.map(attend_block, starts).reshape(TOKENS, HEADS * DH)
    group_rows = HEADS * DH // N_TP
    mixed = jnp.zeros((TOKENS, D), jnp.float32)
    for group_index in range(N_TP):
        lower = group_index * group_rows
        part = jnp.dot(attended[:, lower:lower + group_rows], w_out[lower:lower + group_rows], preferred_element_type=jnp.float32)
        rounded = lax.optimization_barrier(part.astype(jnp.bfloat16))
        mixed = mixed + rounded.astype(jnp.float32)
    normed = layer_norm(ALPHA * residual.astype(jnp.float32) + mixed, norm_gain[0], norm_bias[0])
    blocks = TOKENS // ROWS_DEV
    flat_routes = routing.reshape(blocks, ROWS_DEV * TOP_K)
    one_hot = (flat_routes[..., None] == jnp.arange(EXPERTS, dtype=jnp.int32)[None, None, :]).astype(jnp.int32)
    slot_rank = lax.optimization_barrier(jnp.sum((jnp.cumsum(one_hot, axis=1) - 1) * one_hot, axis=2))
    token_of = (jnp.arange(blocks, dtype=jnp.int32)[:, None] * ROWS_DEV + jnp.arange(ROWS_DEV * TOP_K, dtype=jnp.int32)[None, :] // TOP_K).astype(jnp.int32)
    block_ids = jnp.broadcast_to(jnp.arange(blocks, dtype=jnp.int32)[:, None], flat_routes.shape)
    table = jnp.full((blocks, EXPERTS * CAP), TOKENS, jnp.int32).at[block_ids, flat_routes * CAP + slot_rank].set(token_of)
    table = table.reshape(blocks, EXPERTS, CAP).transpose(1, 0, 2).reshape(EXPERTS, blocks * CAP)
    ff_group = EXPERT_FF // N_TP

    def run_expert(packed):
        index_rows, gate_weight, up_weight, down_weight = packed
        rows = jnp.take(normed, index_rows, axis=0, mode='fill', fill_value=0)
        gate_part = jnp.dot(rows, gate_weight, preferred_element_type=jnp.float32)
        up_part = jnp.dot(rows, up_weight, preferred_element_type=jnp.float32)
        hidden = (jax.nn.silu(gate_part) * up_part).astype(jnp.bfloat16)
        return split_down(hidden, down_weight, ff_group)
    expert_outs = lax.map(run_expert, (table, w_exp_gate, w_exp_up, w_exp_down))
    place = (block_ids * CAP + slot_rank).astype(jnp.int32)
    picked = expert_outs[flat_routes, place].reshape(TOKENS, TOP_K, D).astype(jnp.float32)
    routed = lax.optimization_barrier(jnp.sum(picked * route_weight[:, :, None], axis=1))
    shared_gate = jnp.dot(normed, w_shared_gate, preferred_element_type=jnp.float32)
    shared_up = jnp.dot(normed, w_shared_up, preferred_element_type=jnp.float32)
    shared_hidden = (jax.nn.silu(shared_gate) * shared_up).astype(jnp.bfloat16)
    shared_out = lax.optimization_barrier(split_down(shared_hidden, w_shared_down, SHARED_FF // N_TP))
    combined = routed + shared_out.astype(jnp.float32)
    return layer_norm(ALPHA * normed.astype(jnp.float32) + combined, norm_gain[1], norm_bias[1])
```

```python
import functools

import jax
import jax.numpy as jnp
from jax import lax
from jax.experimental import pallas as pl
from jax.experimental.pallas import tpu as pltpu
from jax.sharding import PartitionSpec as P

LOG2E = 1.4426950408889634
ALPHA = 8.0**0.25
LN_EPS = 1e-05


def in_one_piece(arrays, axis, dim, along):
    both = jnp.concatenate(arrays, axis=along)
    whole, at, done = (lax.all_gather(both, axis, axis=dim, tiled=True), 0, [])
    for a in arrays:
        done.append(lax.slice_in_dim(whole, at, at + a.shape[along], axis=along))
        at += a.shape[along]
    return tuple(done)


def split_up(array, dim, peers):
    dims = array.shape
    blocks = array.reshape(*dims[:dim], peers, dims[dim] // peers, *dims[dim + 1 :])
    return jnp.moveaxis(blocks, dim, 0)


def summed_on_arrival(array, axis, dim):
    peers = lax.axis_size(axis)
    blocks = lax.all_to_all(split_up(array, dim, peers), axis, 0, 0, tiled=True)
    return jnp.sum(blocks.astype(jnp.float32), axis=0)


def sent_to_all(array, axis):
    peers = lax.axis_size(axis)
    return lax.all_to_all(
        jnp.broadcast_to(array[None], (peers, *array.shape)), axis, 0, 0, tiled=True
    )


def joined_along(blocks, dim):
    dims = list(blocks.shape[1:])
    dims[dim] *= blocks.shape[0]
    return jnp.moveaxis(blocks, 0, dim).reshape(dims)


def collect(array, axis, dim):
    blocks = sent_to_all(array, axis)
    return joined_along(blocks, dim)


def layer_norm(summed, gain, shift):
    center = summed - jnp.mean(summed, axis=-1, keepdims=True)
    spread = jnp.mean(center * center, axis=-1, keepdims=True)
    return (center * lax.rsqrt(spread + LN_EPS) * gain + shift).astype(jnp.bfloat16)


def attend_kernel(chunk, sub, off_ref, q_ref, k_ref, v_ref, out_ref, acc):
    me = lax.axis_index("sp")
    rows = q_ref.shape[0]
    heads = off_ref.shape[0]
    dh = k_ref.shape[1]
    scale2 = dh ** -0.5 * LOG2E
    r = lax.broadcasted_iota(jnp.int32, (sub, sub), 0)
    c = lax.broadcasted_iota(jnp.int32, (sub, sub), 1)
    tri = jnp.where(r > c, 1.0, 0.0).astype(jnp.bfloat16)
    last = (me * rows) // chunk
    tpos = me * rows + lax.broadcasted_iota(jnp.int32, (rows, sub), 0)

    def chunk_at(at, carries, masked, first):
        jobs = []
        for j in reversed(range(chunk // sub)):
            base = pl.multiple_of(at * chunk + j * sub, sub)
            k = k_ref[pl.ds(base, sub), :]
            v = v_ref[pl.ds(base, sub), :]
            mask = None
            if masked:
                mask = base + lax.broadcasted_iota(jnp.int32, (rows, sub), 1) < tpos
            for h in range(heads):
                q = q_ref[:, h * dh:(h + 1) * dh]
                s = lax.dot_general(q, k, (((1,), (1,)), ((), ())), preferred_element_type=jnp.float32)
                jobs.append((h, s, v, mask))
        stage = []
        for h, s, v, mask in jobs:
            s = s * scale2 + off_ref[h] * LOG2E
            sp = jnp.maximum(s, 0.0) + jnp.log2(1.0 + jnp.exp2(-jnp.abs(s)))
            own = s - sp
            if mask is not None:
                sp = jnp.where(mask, sp, 0.0)
            hi = sp.astype(jnp.bfloat16)
            lo = (sp - hi.astype(jnp.float32)).astype(jnp.bfloat16)
            after = jnp.dot(hi, tri, preferred_element_type=jnp.float32) + jnp.dot(lo, tri, preferred_element_type=jnp.float32)
            stage.append((h, own - after, after[:, :1] + sp[:, :1], v, mask))
        carries = list(carries)
        parts = [None] * heads
        for h, e, tot, v, mask in stage:
            w = jnp.exp2(e - carries[h])
            if mask is not None:
                w = jnp.where(mask, w, 0.0)
            p = jnp.dot(w.astype(jnp.bfloat16), v, preferred_element_type=jnp.float32)
            parts[h] = p if parts[h] is None else parts[h] + p
            carries[h] = carries[h] + tot
        for h in range(heads):
            sl = slice(h * dh, (h + 1) * dh)
            acc[:, sl] = parts[h] if first else acc[:, sl] + parts[h]
        return tuple(carries)

    carries = chunk_at(last, tuple(jnp.zeros((rows, 1), jnp.float32) for _ in range(heads)), True, True)
    lax.fori_loop(0, last, lambda n, cr: chunk_at(last - 1 - n, cr, False, False), carries)
    out_ref[...] = acc[...].astype(jnp.bfloat16)


def attend(offset, queries, keys, values):
    rows, width = queries.shape
    vmem = pl.BlockSpec(memory_space=pltpu.VMEM)
    return pl.pallas_call(
        functools.partial(attend_kernel, 1024, 256),
        out_shape=jax.ShapeDtypeStruct((rows, width), jnp.bfloat16),
        in_specs=[pl.BlockSpec(memory_space=pltpu.SMEM), vmem, vmem, vmem],
        out_specs=vmem,
        scratch_shapes=[pltpu.VMEM((rows, width), jnp.float32)],
        name="attend",
    )(offset, queries, keys, values)


def per_device(
    residual,
    query_rows,
    key_rows,
    value_rows,
    head_offset,
    w_out,
    norm_gain,
    norm_bias,
    routing,
    route_weight,
    w_exp_gate,
    w_exp_up,
    w_exp_down,
    w_shared_gate,
    w_shared_up,
    w_shared_down,
):
    sp_count = lax.axis_size("sp")
    all_keys, all_values = in_one_piece((key_rows, value_rows), "sp", 0, 1)
    attended = attend(head_offset, query_rows, all_keys, all_values)
    rows_local = residual.shape[0]
    mixed = summed_on_arrival(
        jnp.dot(attended, w_out, preferred_element_type=jnp.float32).astype(jnp.bfloat16), "tp", 0
    )
    normed = layer_norm(ALPHA * residual.astype(jnp.float32) + mixed, norm_gain[0], norm_bias[0])
    top_k = routing.shape[1]
    exp_local = w_exp_gate.shape[0]
    experts = exp_local * sp_count
    capacity = max(2, 3 * rows_local * top_k // (2 * experts))
    flat_routes = routing.reshape(-1)
    one_hot = (flat_routes[:, None] == jnp.arange(experts, dtype=jnp.int32)[None, :]).astype(
        jnp.int32
    )
    slot_rank = jnp.sum((jnp.cumsum(one_hot, axis=0) - 1) * one_hot, axis=1)
    slot_index = flat_routes * capacity + slot_rank
    pair_token = jnp.arange(flat_routes.shape[0], dtype=jnp.int32) // top_k
    source_row = (
        jnp.full((experts * capacity,), rows_local, jnp.int32).at[slot_index].set(pair_token)
    )
    outgoing = jnp.take(normed, source_row, axis=0, mode="fill", fill_value=0)
    outgoing = outgoing.reshape(sp_count, exp_local, capacity, -1)
    arrived = lax.all_to_all(outgoing, "sp", split_axis=0, concat_axis=0, tiled=True)
    routed_rows, token_rows = (collect(arrived, "tp", 0), collect(normed, "tp", 0))
    gate_part = jnp.einsum(
        "aecd,edf->aecf", routed_rows, w_exp_gate, preferred_element_type=jnp.float32
    )
    up_part = jnp.einsum(
        "aecd,edf->aecf", routed_rows, w_exp_up, preferred_element_type=jnp.float32
    )
    hidden = (jax.nn.silu(gate_part) * up_part).astype(jnp.bfloat16)
    expert_part = jnp.einsum(
        "aecf,efd->aecd", hidden, w_exp_down, preferred_element_type=jnp.float32
    )
    shared_gate = jnp.dot(token_rows, w_shared_gate, preferred_element_type=jnp.float32)
    shared_up = jnp.dot(token_rows, w_shared_up, preferred_element_type=jnp.float32)
    shared_hidden = (jax.nn.silu(shared_gate) * shared_up).astype(jnp.bfloat16)
    shared_part = jnp.dot(shared_hidden, w_shared_down, preferred_element_type=jnp.float32)
    expert_sum, shared_sum = (
        summed_on_arrival(expert_part.astype(jnp.bfloat16), "tp", 0),
        summed_on_arrival(shared_part.astype(jnp.bfloat16), "tp", 0),
    )
    returned = lax.all_to_all(
        expert_sum.astype(jnp.bfloat16), "sp", split_axis=0, concat_axis=0, tiled=True
    )
    returned = returned.reshape(experts * capacity, -1)
    picked = returned[slot_index].astype(jnp.float32).reshape(rows_local, top_k, -1)
    routed = jnp.sum(picked * route_weight[:, :, None], axis=1)
    shared_out = lax.optimization_barrier(shared_sum.astype(jnp.bfloat16))
    combined = routed + shared_out.astype(jnp.float32)
    return layer_norm(ALPHA * normed.astype(jnp.float32) + combined, norm_gain[1], norm_bias[1])


def solution(mesh):
    placed = (
        P(("sp", "tp"), None),
        P("sp", "tp"),
        P("sp", "tp"),
        P("sp", "tp"),
        P("tp"),
        P("tp", None),
        P(),
        P(),
        P(("sp", "tp"), None),
        P(("sp", "tp"), None),
        P("sp", None, "tp"),
        P("sp", None, "tp"),
        P("sp", "tp", None),
        P(None, "tp"),
        P(None, "tp"),
        P("tp", None),
    )
    return jax.shard_map(
        per_device, mesh=mesh, in_specs=placed, out_specs=P(("sp", "tp"), None), check_vma=False
    )
```

```python
import functools

import jax
import jax.numpy as jnp
from jax import lax
from jax.experimental import pallas as pl
from jax.experimental.pallas import tpu as pltpu
from jax.sharding import PartitionSpec as P

LOG2E = 1.4426950408889634
ALPHA = 8.0**0.25
LN_EPS = 1e-05


def split_up(array, dim, peers):
    dims = array.shape
    blocks = array.reshape(*dims[:dim], peers, dims[dim] // peers, *dims[dim + 1 :])
    return jnp.moveaxis(blocks, dim, 0)


def summed_on_arrival(array, axis, dim):
    peers = lax.axis_size(axis)
    blocks = lax.all_to_all(split_up(array, dim, peers), axis, 0, 0, tiled=True)
    return jnp.sum(blocks.astype(jnp.float32), axis=0)


def sent_to_all(array, axis):
    peers = lax.axis_size(axis)
    return lax.all_to_all(
        jnp.broadcast_to(array[None], (peers, *array.shape)), axis, 0, 0, tiled=True
    )


def joined_along(blocks, dim):
    dims = list(blocks.shape[1:])
    dims[dim] *= blocks.shape[0]
    return jnp.moveaxis(blocks, 0, dim).reshape(dims)


def collect(array, axis, dim):
    blocks = sent_to_all(array, axis)
    return joined_along(blocks, dim)


def layer_norm(summed, gain, shift):
    center = summed - jnp.mean(summed, axis=-1, keepdims=True)
    spread = jnp.mean(center * center, axis=-1, keepdims=True)
    return (center * lax.rsqrt(spread + LN_EPS) * gain + shift).astype(jnp.bfloat16)


def cross(sp_count):
    rows_x = 4
    return sp_count // (2 * rows_x), rows_x


def attend_kernel(rows_z, rows_x, off_ref, q_ref, k_ref, v_ref, out_ref,
                  keys, values, right, left, carry, send, recv, local):
    me = lax.axis_index("sp")
    z, x, c = (
        lax.div(me, 2 * rows_x),
        lax.rem(lax.div(me, 2), rows_x),
        lax.rem(me, 2),
    )
    rows = q_ref.shape[0]
    heads = off_ref.shape[0]
    dh = k_ref.shape[1]
    half = rows // 2
    reach = rows_z // 2

    def at(zz, xx, cc):
        return (zz * rows_x + xx) * 2 + cc

    def turn(value, by, size):
        return lax.rem(value + (by + size), size)

    z_up, z_down = turn(z, 1, rows_z), turn(z, -1, rows_z)
    x_up, x_down = turn(x, 1, rows_x), turn(x, -1, rows_x)
    x_far = turn(x, 2, rows_x)
    to_z = {1: at(z_up, x, c), -1: at(z_down, x, c)}
    to_x = {1: at(z, x_up, c), -1: at(z, x_down, c)}
    partner = at(z, x, 1 - c)

    names = {}

    def copy(name, src, dst, target):
        slot = names.setdefault(name, len(names))
        return pltpu.make_async_remote_copy(
            src_ref=src, dst_ref=dst, send_sem=send.at[slot], recv_sem=recv.at[slot],
            device_id={"sp": target}, device_id_type=pl.DeviceIdType.MESH,
        )

    started = []

    def begin(*args):
        job = copy(*args)
        job.start()
        started.append(job)

    def arrive(name, dst):
        copy(name, dst, dst, partner).wait_recv()

    barrier = pltpu.get_barrier_semaphore()
    peers = (to_z[1], to_z[-1], to_x[1], to_x[-1], partner)
    for peer in peers:
        pl.semaphore_signal(barrier, inc=1, device_id={"sp": peer}, device_id_type=pl.DeviceIdType.MESH)
    pl.semaphore_wait(barrier, len(peers))

    keep_k = pltpu.make_async_copy(k_ref, keys.at[z, x, c], local.at[0])
    keep_v = pltpu.make_async_copy(v_ref, values.at[z, x, c], local.at[1])
    keep_k.start()
    keep_v.start()
    own_k, own_v = keys.at[z, x, c], values.at[z, x, c]
    for way in (1, -1):
        begin(("kx", way), k_ref, own_k, to_x[way])
    for way in (1, -1):
        begin(("vz", way, 1), v_ref, own_v, to_z[way])
    for way in (1, -1):
        begin(("vx", 0, 0, way), v_ref, own_v, to_x[way])

    lower, upper = pl.ds(0, half), pl.ds(half, half)
    side = {1: x_down, -1: x_up}
    part = {1: lower, -1: upper}

    def across(tag, buf, zz):
        for way in (1, -1):
            arrive(tag + (way,), buf.at[zz, side[way], c])
            piece = buf.at[zz, side[way], c, part[way]]
            begin(tag + ("far", way), piece, piece, to_x[way])

    def across_end(tag, buf, zz):
        for way in (1, -1):
            arrive(tag + ("far", way), buf.at[zz, x_far, c, part[way]])

    def share(tag, buf, zz):
        begin(tag + ("peer",), buf.at[zz, :, c], buf.at[zz, :, c], partner)

    def shared(tag, buf, zz):
        other = buf.at[zz, :, 1 - c]
        arrive(tag + ("peer",), other)

    pieces = {0: pl.ds(0, rows_x // 2), 1: pl.ds(rows_x // 2, rows_x // 2)}

    def forward_k(way, zz, step):
        for sub in (0, 1):
            if step == reach and (sub == 0) != (way == 1):
                continue
            block = keys.at[zz, pieces[sub], c]
            begin(("kz", way, step, sub), block, block, to_z[way])

    across(("kx",), keys, z)
    keep_k.wait()
    keep_v.wait()
    across_end(("kx",), keys, z)
    for way in (1, -1):
        forward_k(way, z, 1)
    share(("k", 0, 0), keys, z)

    def slab_of(way, step):
        return turn(z, -way * step, rows_z)

    def z_step_v(step):
        for way in (1, -1):
            zz = slab_of(way, step)
            if step < reach:
                block = values.at[zz, x, c]
                arrive(("vz", way, step), block)
                if step + 1 < reach:
                    begin(("vz", way, step + 1), block, block, to_z[way])
                else:
                    piece = values.at[zz, x, c, part[way]]
                    begin(("vz", way, step + 1), piece, piece, to_z[way])
                for side_way in (1, -1):
                    begin(("vx", way, step, side_way), block, block, to_x[side_way])
            else:
                piece = values.at[zz, x, c, part[way]]
                arrive(("vz", way, step), piece)
        if step == reach:
            block = values.at[slab_of(1, step), x, c]
            for side_way in (1, -1):
                begin(("vx", 1, step, side_way), block, block, to_x[side_way])

    def slabs_at(step):
        if step == 0:
            return ((0, 0),)
        if step == reach:
            return ((1, step),)
        return ((1, step), (-1, step))

    def z_step_k(step):
        for way in (1, -1):
            zz = slab_of(way, step)
            for sub in (0, 1):
                if step == reach and (sub == 0) != (way == 1):
                    continue
                arrive(("kz", way, step, sub), keys.at[zz, pieces[sub], c])
            if step < reach:
                forward_k(way, zz, step + 1)
        for way, stp in slabs_at(step):
            share(("k", way, stp), keys, slab_of(way, stp))

    scale2 = dh**-0.5 * LOG2E
    sub = 2 * rows
    r_at = lax.broadcasted_iota(jnp.int32, (sub, sub), 0)
    c_at = lax.broadcasted_iota(jnp.int32, (sub, sub), 1)
    after_of = jnp.where(r_at > c_at, 1.0, 0.0).astype(jnp.bfloat16)
    t_in_slab = (x * 2 + c) * rows + lax.broadcasted_iota(jnp.int32, (rows, sub), 0)

    def slab(zz, carries, masked):
        stage = []
        for j in reversed(range(rows_x)):
            k = keys[zz, j].reshape(sub, dh)
            v = values[zz, j].reshape(sub, dh)
            mask = None
            if masked:
                mask = j * sub + lax.broadcasted_iota(jnp.int32, (rows, sub), 1) < t_in_slab
            for h in range(heads):
                q = q_ref[:, h * dh : (h + 1) * dh]
                s = lax.dot_general(q, k, (((1,), (1,)), ((), ())), preferred_element_type=jnp.float32)
                s = s * scale2 + off_ref[h] * LOG2E
                sp = jnp.maximum(s, 0.0) + jnp.log2(1.0 + jnp.exp2(-jnp.abs(s)))
                own = s - sp
                if masked:
                    sp = jnp.where(mask, sp, 0.0)
                hi = sp.astype(jnp.bfloat16)
                lo = (sp - hi.astype(jnp.float32)).astype(jnp.bfloat16)
                after = jnp.dot(hi, after_of, preferred_element_type=jnp.float32)
                after = after + jnp.dot(lo, after_of, preferred_element_type=jnp.float32)
                stage.append((h, own - after, after[:, :1] + sp[:, :1], v, mask))
        carries = list(carries)
        parts = [None] * heads
        for h, exponent, total, v, mask in stage:
            w = jnp.exp2(exponent - carries[h])
            if masked:
                w = jnp.where(mask, w, 0.0)
            piece = jnp.dot(w.astype(jnp.bfloat16), v, preferred_element_type=jnp.float32)
            parts[h] = piece if parts[h] is None else parts[h] + piece
            carries[h] = carries[h] + total
        return parts, carries

    def columns(h):
        return slice(h * dh, (h + 1) * dh)

    def put_carry(carries):
        for h in range(heads):
            carry[h] = jnp.broadcast_to(carries[h], (rows, dh))

    def own_slab():
        parts, carries = slab(z, [jnp.zeros((rows, 1), jnp.float32)] * heads, True)
        for h in range(heads):
            right[:, columns(h)] = parts[h]
        put_carry(carries)
        left[...] = jnp.zeros_like(left)

    def right_slab(step):
        @pl.when(z >= step)
        def _():
            parts, carries = slab(z - step, [carry[h][:, :1] for h in range(heads)], False)
            for h in range(heads):
                right[:, columns(h)] = right[:, columns(h)] + parts[h]
            put_carry(carries)

    def left_slab(step):
        @pl.when(z + step >= rows_z)
        def _():
            parts, totals = slab(z + step - rows_z, [jnp.zeros((rows, 1), jnp.float32)] * heads, False)
            for h in range(heads):
                left[:, columns(h)] = parts[h] + jnp.exp2(-totals[h]) * left[:, columns(h)]

    for step in range(reach + 1):
        if step > 0:
            z_step_k(step)
        for way, stp in slabs_at(step):
            across(("vx", way, stp), values, slab_of(way, stp))
        if step < reach:
            z_step_v(step + 1)
        for way, stp in slabs_at(step):
            across_end(("vx", way, stp), values, slab_of(way, stp))
            share(("v", way, stp), values, slab_of(way, stp))
        ready = step - 1 if step < reach else None
        for done in ([step - 1] if step > 0 else []) + ([reach] if step == reach else []):
            for way, stp in slabs_at(done):
                shared(("k", way, stp), keys, slab_of(way, stp))
                shared(("v", way, stp), values, slab_of(way, stp))
            if done == 0:
                own_slab()
            else:
                right_slab(done)
                if done < reach:
                    left_slab(done)
    for h in range(heads):
        cols = columns(h)
        out_ref[:, cols] = (right[:, cols] + jnp.exp2(-carry[h]) * left[:, cols]).astype(jnp.bfloat16)
    for job in started:
        job.wait_send()


def attend(offset, queries, keys, values):
    rows, width = queries.shape
    dh = keys.shape[1]
    heads = offset.shape[0]
    rows_z, rows_x = cross(lax.axis_size("sp"))
    vmem = pl.BlockSpec(memory_space=pltpu.VMEM)
    whole = pltpu.VMEM((rows_z, rows_x, 2, rows, dh), jnp.bfloat16)
    return pl.pallas_call(
        functools.partial(attend_kernel, rows_z, rows_x),
        out_shape=jax.ShapeDtypeStruct((rows, width), jnp.bfloat16),
        in_specs=[pl.BlockSpec(memory_space=pltpu.SMEM), vmem, vmem, vmem],
        out_specs=vmem,
        scratch_shapes=[
            whole,
            whole,
            pltpu.VMEM((rows, width), jnp.float32),
            pltpu.VMEM((rows, width), jnp.float32),
            pltpu.VMEM((heads, rows, dh), jnp.float32),
            pltpu.SemaphoreType.DMA((96,)),
            pltpu.SemaphoreType.DMA((96,)),
            pltpu.SemaphoreType.DMA((2,)),
        ],
        compiler_params=pltpu.CompilerParams(collective_id=0, has_side_effects=True),
        name="attend",
    )(offset, queries, keys, values)


def per_device(
    residual,
    query_rows,
    key_rows,
    value_rows,
    head_offset,
    w_out,
    norm_gain,
    norm_bias,
    routing,
    route_weight,
    w_exp_gate,
    w_exp_up,
    w_exp_down,
    w_shared_gate,
    w_shared_up,
    w_shared_down,
):
    sp_count = lax.axis_size("sp")
    attended = attend(head_offset, query_rows, key_rows, value_rows)
    rows_local = residual.shape[0]
    mixed = summed_on_arrival(
        jnp.dot(attended, w_out, preferred_element_type=jnp.float32).astype(jnp.bfloat16), "tp", 0
    )
    normed = layer_norm(ALPHA * residual.astype(jnp.float32) + mixed, norm_gain[0], norm_bias[0])
    top_k = routing.shape[1]
    exp_local = w_exp_gate.shape[0]
    experts = exp_local * sp_count
    capacity = max(2, 3 * rows_local * top_k // (2 * experts))
    flat_routes = routing.reshape(-1)
    one_hot = (flat_routes[:, None] == jnp.arange(experts, dtype=jnp.int32)[None, :]).astype(
        jnp.int32
    )
    slot_rank = jnp.sum((jnp.cumsum(one_hot, axis=0) - 1) * one_hot, axis=1)
    slot_index = flat_routes * capacity + slot_rank
    pair_token = jnp.arange(flat_routes.shape[0], dtype=jnp.int32) // top_k
    source_row = (
        jnp.full((experts * capacity,), rows_local, jnp.int32).at[slot_index].set(pair_token)
    )
    outgoing = jnp.take(normed, source_row, axis=0, mode="fill", fill_value=0)
    outgoing = outgoing.reshape(sp_count, exp_local, capacity, -1)
    arrived = lax.all_to_all(outgoing, "sp", split_axis=0, concat_axis=0, tiled=True)
    routed_rows, token_rows = (collect(arrived, "tp", 0), collect(normed, "tp", 0))
    gate_part = jnp.einsum(
        "aecd,edf->aecf", routed_rows, w_exp_gate, preferred_element_type=jnp.float32
    )
    up_part = jnp.einsum(
        "aecd,edf->aecf", routed_rows, w_exp_up, preferred_element_type=jnp.float32
    )
    hidden = (jax.nn.silu(gate_part) * up_part).astype(jnp.bfloat16)
    expert_part = jnp.einsum(
        "aecf,efd->aecd", hidden, w_exp_down, preferred_element_type=jnp.float32
    )
    shared_gate = jnp.dot(token_rows, w_shared_gate, preferred_element_type=jnp.float32)
    shared_up = jnp.dot(token_rows, w_shared_up, preferred_element_type=jnp.float32)
    shared_hidden = (jax.nn.silu(shared_gate) * shared_up).astype(jnp.bfloat16)
    shared_part = jnp.dot(shared_hidden, w_shared_down, preferred_element_type=jnp.float32)
    expert_sum, shared_sum = (
        summed_on_arrival(expert_part.astype(jnp.bfloat16), "tp", 0),
        summed_on_arrival(shared_part.astype(jnp.bfloat16), "tp", 0),
    )
    returned = lax.all_to_all(
        expert_sum.astype(jnp.bfloat16), "sp", split_axis=0, concat_axis=0, tiled=True
    )
    returned = returned.reshape(experts * capacity, -1)
    picked = returned[slot_index].astype(jnp.float32).reshape(rows_local, top_k, -1)
    routed = jnp.sum(picked * route_weight[:, :, None], axis=1)
    shared_out = lax.optimization_barrier(shared_sum.astype(jnp.bfloat16))
    combined = routed + shared_out.astype(jnp.float32)
    return layer_norm(ALPHA * normed.astype(jnp.float32) + combined, norm_gain[1], norm_bias[1])


def solution(mesh):
    placed = (
        P(("sp", "tp"), None),
        P("sp", "tp"),
        P("sp", "tp"),
        P("sp", "tp"),
        P("tp"),
        P("tp", None),
        P(),
        P(),
        P(("sp", "tp"), None),
        P(("sp", "tp"), None),
        P("sp", None, "tp"),
        P("sp", None, "tp"),
        P("sp", "tp", None),
        P(None, "tp"),
        P(None, "tp"),
        P("tp", None),
    )
    return jax.shard_map(
        per_device, mesh=mesh, in_specs=placed, out_specs=P(("sp", "tp"), None), check_vma=False
    )
```

```python
import functools

import jax
import jax.numpy as jnp
from jax import lax
from jax.experimental import pallas as pl
from jax.experimental.pallas import tpu as pltpu
from jax.sharding import PartitionSpec as P

LOG2E = 1.4426950408889634
ALPHA = 8.0**0.25
LN_EPS = 1e-05


def cross(sp_count):
    rows_x = 4
    return sp_count // (2 * rows_x), rows_x


def attend_kernel(rows_z, rows_x, off_ref, q_ref, k_ref, v_ref, out_ref,
                  keys, values, right, left, carry, send, recv, local):
    me = lax.axis_index("sp")
    z, x, c = (
        lax.div(me, 2 * rows_x),
        lax.rem(lax.div(me, 2), rows_x),
        lax.rem(me, 2),
    )
    rows = q_ref.shape[0]
    heads = off_ref.shape[0]
    dh = k_ref.shape[1]
    half = rows // 2
    reach = rows_z // 2

    def at(zz, xx, cc):
        return (zz * rows_x + xx) * 2 + cc

    def turn(value, by, size):
        return lax.rem(value + (by + size), size)

    z_up, z_down = turn(z, 1, rows_z), turn(z, -1, rows_z)
    x_up, x_down = turn(x, 1, rows_x), turn(x, -1, rows_x)
    x_far = turn(x, 2, rows_x)
    to_z = {1: at(z_up, x, c), -1: at(z_down, x, c)}
    to_x = {1: at(z, x_up, c), -1: at(z, x_down, c)}
    partner = at(z, x, 1 - c)

    names = {}

    def copy(name, src, dst, target):
        slot = names.setdefault(name, len(names))
        return pltpu.make_async_remote_copy(
            src_ref=src, dst_ref=dst, send_sem=send.at[slot], recv_sem=recv.at[slot],
            device_id={"sp": target}, device_id_type=pl.DeviceIdType.MESH,
        )

    started = []

    def begin(*args):
        job = copy(*args)
        job.start()
        started.append(job)

    def arrive(name, dst):
        copy(name, dst, dst, partner).wait_recv()

    barrier = pltpu.get_barrier_semaphore()
    peers = (to_z[1], to_z[-1], to_x[1], to_x[-1], partner)
    for peer in peers:
        pl.semaphore_signal(barrier, inc=1, device_id={"sp": peer}, device_id_type=pl.DeviceIdType.MESH)
    pl.semaphore_wait(barrier, len(peers))

    keep_k = pltpu.make_async_copy(k_ref, keys.at[z, x, c], local.at[0])
    keep_v = pltpu.make_async_copy(v_ref, values.at[z, x, c], local.at[1])
    keep_k.start()
    keep_v.start()
    own_k, own_v = keys.at[z, x, c], values.at[z, x, c]
    for way in (1, -1):
        begin(("kx", way), k_ref, own_k, to_x[way])
    for way in (1, -1):
        begin(("vz", way, 1), v_ref, own_v, to_z[way])
    for way in (1, -1):
        begin(("vx", 0, 0, way), v_ref, own_v, to_x[way])

    lower, upper = pl.ds(0, half), pl.ds(half, half)
    side = {1: x_down, -1: x_up}
    part = {1: lower, -1: upper}

    def across(tag, buf, zz):
        for way in (1, -1):
            arrive(tag + (way,), buf.at[zz, side[way], c])
            piece = buf.at[zz, side[way], c, part[way]]
            begin(tag + ("far", way), piece, piece, to_x[way])

    def across_end(tag, buf, zz):
        for way in (1, -1):
            arrive(tag + ("far", way), buf.at[zz, x_far, c, part[way]])

    def share(tag, buf, zz):
        begin(tag + ("peer",), buf.at[zz, :, c], buf.at[zz, :, c], partner)

    def shared(tag, buf, zz):
        other = buf.at[zz, :, 1 - c]
        arrive(tag + ("peer",), other)

    pieces = {0: pl.ds(0, rows_x // 2), 1: pl.ds(rows_x // 2, rows_x // 2)}

    def forward_k(way, zz, step):
        for sub in (0, 1):
            if step == reach and (sub == 0) != (way == 1):
                continue
            block = keys.at[zz, pieces[sub], c]
            begin(("kz", way, step, sub), block, block, to_z[way])

    across(("kx",), keys, z)
    keep_k.wait()
    keep_v.wait()
    across_end(("kx",), keys, z)
    for way in (1, -1):
        forward_k(way, z, 1)
    share(("k", 0, 0), keys, z)

    def slab_of(way, step):
        return turn(z, -way * step, rows_z)

    def z_step_v(step):
        for way in (1, -1):
            zz = slab_of(way, step)
            if step < reach:
                block = values.at[zz, x, c]
                arrive(("vz", way, step), block)
                if step + 1 < reach:
                    begin(("vz", way, step + 1), block, block, to_z[way])
                else:
                    piece = values.at[zz, x, c, part[way]]
                    begin(("vz", way, step + 1), piece, piece, to_z[way])
                for side_way in (1, -1):
                    begin(("vx", way, step, side_way), block, block, to_x[side_way])
            else:
                piece = values.at[zz, x, c, part[way]]
                arrive(("vz", way, step), piece)
        if step == reach:
            block = values.at[slab_of(1, step), x, c]
            for side_way in (1, -1):
                begin(("vx", 1, step, side_way), block, block, to_x[side_way])

    def slabs_at(step):
        if step == 0:
            return ((0, 0),)
        if step == reach:
            return ((1, step),)
        return ((1, step), (-1, step))

    def z_step_k(step):
        for way in (1, -1):
            zz = slab_of(way, step)
            for sub in (0, 1):
                if step == reach and (sub == 0) != (way == 1):
                    continue
                arrive(("kz", way, step, sub), keys.at[zz, pieces[sub], c])
            if step < reach:
                forward_k(way, zz, step + 1)
        for way, stp in slabs_at(step):
            share(("k", way, stp), keys, slab_of(way, stp))

    scale2 = dh**-0.5 * LOG2E
    sub = 2 * rows
    r_at = lax.broadcasted_iota(jnp.int32, (sub, sub), 0)
    c_at = lax.broadcasted_iota(jnp.int32, (sub, sub), 1)
    after_of = jnp.where(r_at > c_at, 1.0, 0.0).astype(jnp.bfloat16)
    t_in_slab = (x * 2 + c) * rows + lax.broadcasted_iota(jnp.int32, (rows, sub), 0)

    def slab(zz, carries, masked):
        stage = []
        for j in reversed(range(rows_x)):
            k = keys[zz, j].reshape(sub, dh)
            v = values[zz, j].reshape(sub, dh)
            mask = None
            if masked:
                mask = j * sub + lax.broadcasted_iota(jnp.int32, (rows, sub), 1) < t_in_slab
            for h in range(heads):
                q = q_ref[:, h * dh : (h + 1) * dh]
                s = lax.dot_general(q, k, (((1,), (1,)), ((), ())), preferred_element_type=jnp.float32)
                s = s * scale2 + off_ref[h] * LOG2E
                sp = jnp.maximum(s, 0.0) + jnp.log2(1.0 + jnp.exp2(-jnp.abs(s)))
                own = s - sp
                if masked:
                    sp = jnp.where(mask, sp, 0.0)
                hi = sp.astype(jnp.bfloat16)
                lo = (sp - hi.astype(jnp.float32)).astype(jnp.bfloat16)
                after = jnp.dot(hi, after_of, preferred_element_type=jnp.float32)
                after = after + jnp.dot(lo, after_of, preferred_element_type=jnp.float32)
                stage.append((h, own - after, after[:, :1] + sp[:, :1], v, mask))
        carries = list(carries)
        parts = [None] * heads
        for h, exponent, total, v, mask in stage:
            w = jnp.exp2(exponent - carries[h])
            if masked:
                w = jnp.where(mask, w, 0.0)
            piece = jnp.dot(w.astype(jnp.bfloat16), v, preferred_element_type=jnp.float32)
            parts[h] = piece if parts[h] is None else parts[h] + piece
            carries[h] = carries[h] + total
        return parts, carries

    def columns(h):
        return slice(h * dh, (h + 1) * dh)

    def put_carry(carries):
        for h in range(heads):
            carry[h] = jnp.broadcast_to(carries[h], (rows, dh))

    def own_slab():
        parts, carries = slab(z, [jnp.zeros((rows, 1), jnp.float32)] * heads, True)
        for h in range(heads):
            right[:, columns(h)] = parts[h]
        put_carry(carries)
        left[...] = jnp.zeros_like(left)

    def right_slab(step):
        @pl.when(z >= step)
        def _():
            parts, carries = slab(z - step, [carry[h][:, :1] for h in range(heads)], False)
            for h in range(heads):
                right[:, columns(h)] = right[:, columns(h)] + parts[h]
            put_carry(carries)

    def left_slab(step):
        @pl.when(z + step >= rows_z)
        def _():
            parts, totals = slab(z + step - rows_z, [jnp.zeros((rows, 1), jnp.float32)] * heads, False)
            for h in range(heads):
                left[:, columns(h)] = parts[h] + jnp.exp2(-totals[h]) * left[:, columns(h)]

    for step in range(reach + 1):
        if step > 0:
            z_step_k(step)
        for way, stp in slabs_at(step):
            across(("vx", way, stp), values, slab_of(way, stp))
        if step < reach:
            z_step_v(step + 1)
        for way, stp in slabs_at(step):
            across_end(("vx", way, stp), values, slab_of(way, stp))
            share(("v", way, stp), values, slab_of(way, stp))
        ready = step - 1 if step < reach else None
        for done in ([step - 1] if step > 0 else []) + ([reach] if step == reach else []):
            for way, stp in slabs_at(done):
                shared(("k", way, stp), keys, slab_of(way, stp))
                shared(("v", way, stp), values, slab_of(way, stp))
            if done == 0:
                own_slab()
            else:
                right_slab(done)
                if done < reach:
                    left_slab(done)
    for h in range(heads):
        cols = columns(h)
        out_ref[:, cols] = (right[:, cols] + jnp.exp2(-carry[h]) * left[:, cols]).astype(jnp.bfloat16)
    for job in started:
        job.wait_send()


def attend(offset, queries, keys, values):
    rows, width = queries.shape
    dh = keys.shape[1]
    heads = offset.shape[0]
    rows_z, rows_x = cross(lax.axis_size("sp"))
    vmem = pl.BlockSpec(memory_space=pltpu.VMEM)
    whole = pltpu.VMEM((rows_z, rows_x, 2, rows, dh), jnp.bfloat16)
    return pl.pallas_call(
        functools.partial(attend_kernel, rows_z, rows_x),
        out_shape=jax.ShapeDtypeStruct((rows, width), jnp.bfloat16),
        in_specs=[pl.BlockSpec(memory_space=pltpu.SMEM), vmem, vmem, vmem],
        out_specs=vmem,
        scratch_shapes=[
            whole,
            whole,
            pltpu.VMEM((rows, width), jnp.float32),
            pltpu.VMEM((rows, width), jnp.float32),
            pltpu.VMEM((heads, rows, dh), jnp.float32),
            pltpu.SemaphoreType.DMA((96,)),
            pltpu.SemaphoreType.DMA((96,)),
            pltpu.SemaphoreType.DMA((2,)),
        ],
        compiler_params=pltpu.CompilerParams(collective_id=0, has_side_effects=True),
        name="attend",
    )(offset, queries, keys, values)


def moe_kernel(rows_z, chunks, capacity,
               att_ref, res_ref, route_ref, rw_ref, gain_ref, bias_ref,
               wo_hbm, wg_hbm, wu_hbm, wd_hbm, sg_hbm, su_hbm, sd_hbm,
               out_ref,
               wo, wg, wu, wd, sg, su, sd,
               proj, proj_far, proj_in, normed, tokens,
               out_z, in_z, out_x, rows_all, gate, up, shared_hidden, hidden,
               part, part_far, part_in, back_x, in_bx, back_z, in_bz, shared_sum, total,
               send, recv, local):
    me = lax.axis_index("sp")
    y = lax.axis_index("tp")
    group = lax.axis_size("sp") // rows_z
    z, w = lax.div(me, group), lax.rem(me, group)
    tp = lax.axis_size("tp")
    block = rows_z * capacity
    rows, width = res_ref.shape
    slots = out_z.shape[0]
    cols = width // chunks
    mesh_ids = pl.DeviceIdType.MESH

    def turn(value, by, size):
        return lax.rem(value + (by + size), size)

    y_side = {1: turn(y, 1, tp), -1: turn(y, -1, tp)}
    y_far = turn(y, 2, tp)

    barrier = pltpu.get_barrier_semaphore()
    peers = [{"sp": turn(z, d, rows_z) * group + w} for d in range(1, rows_z)]
    peers += [{"sp": z * group + turn(w, d, group)} for d in range(1, group)]
    peers += [{"tp": y_side[1]}, {"tp": y_side[-1]}]
    for peer in peers:
        pl.semaphore_signal(barrier, inc=1, device_id=peer, device_id_type=mesh_ids)

    loads = []
    for i, (src, dst) in enumerate((
        (wo_hbm, wo), (sg_hbm, sg), (su_hbm, su), (wg_hbm.at[0], wg), (wu_hbm.at[0], wu),
        (wd_hbm.at[0], wd), (sd_hbm, sd),
    )):
        load = pltpu.make_async_copy(src, dst, local.at[i])
        load.start()
        loads.append(load)

    names = {}
    started = []

    def copy(name, src, dst, target):
        slot = names.setdefault(name, len(names))
        return pltpu.make_async_remote_copy(
            src_ref=src, dst_ref=dst, send_sem=send.at[slot], recv_sem=recv.at[slot],
            device_id=target, device_id_type=mesh_ids,
        )

    def begin(name, src, dst, target):
        job = copy(name, src, dst, target)
        job.start()
        started.append(job)

    def arrive(name, dst):
        copy(name, dst, dst, {"tp": y_side[1]}).wait_recv()

    def to_y(way):
        return {"tp": y_side[way]}

    loads[0].wait()
    for j in range(tp):
        proj[j] = jnp.dot(
            att_ref[j * rows : (j + 1) * rows, :], wo[...], preferred_element_type=jnp.float32
        ).astype(jnp.bfloat16)
    pl.semaphore_wait(barrier, len(peers))

    def halves(n):
        return {1: pl.ds(0, n // 2), -1: pl.ds(n // 2, n // 2)}

    def sum_far(tag, src, far, at):
        piece = halves(src.shape[1])
        for way in (1, -1):
            begin((tag, "far", way), at(src.at[y_far, piece[way]]), at(far.at[0 if way == 1 else 1]), to_y(way))

    def sum_pass(tag, src, far, arrived, at):
        piece = halves(src.shape[1])
        for way in (1, -1):
            got = at(far.at[0 if way == 1 else 1])
            arrive((tag, "far", way), got)
            mine = at(src.at[y_side[way], piece[way]])
            mine[...] = (mine[...].astype(jnp.float32) + got[...].astype(jnp.float32)).astype(jnp.bfloat16)
            begin((tag, "near", way), at(src.at[y_side[way]]), at(arrived.at[0 if way == 1 else 1]), to_y(way))

    def sum_done(tag, src, arrived, at):
        acc = at(src.at[y])[...].astype(jnp.float32)
        for way in (1, -1):
            got = at(arrived.at[0 if way == 1 else 1])
            arrive((tag, "near", way), got)
            acc = acc + got[...].astype(jnp.float32)
        return acc

    def spread(tag, buf, at):
        for way in (1, -1):
            begin((tag, "near", way), at(buf.at[y]), at(buf.at[y]), to_y(way))

    def spread_pass(tag, buf, at):
        piece = halves(buf.shape[1])
        for way in (1, -1):
            side = y_side[-way]
            arrive((tag, "near", way), at(buf.at[side]))
            half = at(buf.at[side, piece[way]])
            begin((tag, "far", way), half, half, to_y(way))

    def spread_done(tag, buf, at):
        piece = halves(buf.shape[1])
        for way in (1, -1):
            arrive((tag, "far", way), at(buf.at[y_far, piece[way]]))

    def all_of(ref):
        return ref

    def chunk_of(q):
        return lambda ref: ref.at[:, pl.ds(q * cols, cols)]

    sum_far("proj", proj, proj_far, all_of)

    t_row = lax.broadcasted_iota(jnp.int32, (rows, rows), 0)
    t_col = lax.broadcasted_iota(jnp.int32, (rows, rows), 1)
    routes = route_ref[...].astype(jnp.float32)
    e_col = [routes[:, k : k + 1] for k in (0, 1)]
    e_row = [jnp.sum(jnp.where(t_row == t_col, e, 0.0), axis=0, keepdims=True) for e in e_col]

    def same(a, b, keep=None):
        hit = jnp.where(a == b, 1.0, 0.0)
        return hit if keep is None else jnp.where(keep, hit, 0.0)

    rank_col = [
        jnp.sum(same(e_col[0], e_row[0], t_col < t_row), axis=1, keepdims=True),
        jnp.sum(same(e_col[1], e_row[0]) + same(e_col[1], e_row[1], t_col < t_row), axis=1, keepdims=True),
    ]
    rank_row = [
        jnp.sum(same(e_col[0], e_row[0], t_row < t_col), axis=0, keepdims=True),
        jnp.sum(same(e_col[0], e_row[1]) + same(e_col[1], e_row[1], t_row < t_col), axis=0, keepdims=True),
    ]
    slot_col = [e_col[k] * capacity + rank_col[k] for k in (0, 1)]
    slot_row = [e_row[k] * capacity + rank_row[k] for k in (0, 1)]
    s_row = lax.broadcasted_iota(jnp.int32, (slots, rows), 0).astype(jnp.float32)
    place = (same(s_row, slot_row[0]) + same(s_row, slot_row[1])).astype(jnp.bfloat16)
    s_col = lax.broadcasted_iota(jnp.int32, (rows, slots), 1).astype(jnp.float32)
    pick = [same(s_col, slot_col[k]).astype(jnp.bfloat16) for k in (0, 1)]
    i_dst = lax.broadcasted_iota(jnp.int32, (slots, slots), 0)
    i_src = lax.broadcasted_iota(jnp.int32, (slots, slots), 1)
    from_row = lax.div(lax.rem(i_dst, block), capacity) * block + lax.div(i_dst, block) * capacity + lax.rem(i_dst, capacity)
    swap = jnp.where(i_src == from_row, 1.0, 0.0).astype(jnp.bfloat16)

    def norm(summed, n):
        center = summed - jnp.mean(summed, axis=-1, keepdims=True)
        spread_ = jnp.mean(center * center, axis=-1, keepdims=True)
        scaled = center * lax.rsqrt(spread_ + LN_EPS) * gain_ref[n : n + 1, :] + bias_ref[n : n + 1, :]
        return scaled.astype(jnp.bfloat16)

    sum_pass("proj", proj, proj_far, proj_in, all_of)
    mixed = sum_done("proj", proj, proj_in, all_of)
    normed[...] = norm(ALPHA * res_ref[...].astype(jnp.float32) + mixed, 0)
    tokens[y] = normed[...]

    def rows_at(n):
        return pl.ds(pl.multiple_of(n * block, block), block)

    def exchange(tag, q, axis, outgoing, incoming):
        here, size = (z, rows_z) if axis == "z" else (w, group)
        span = pl.ds(q * cols, cols)
        for d in range(1, size):
            there = turn(here, d, size)
            target = {"sp": there * group + w} if axis == "z" else {"sp": z * group + there}
            begin((tag, q, d), outgoing.at[rows_at(there), span], incoming.at[rows_at(here), span], target)
        incoming[rows_at(here), span] = outgoing[rows_at(here), span]

    def exchanged(tag, q, axis, incoming):
        here, size = (z, rows_z) if axis == "z" else (w, group)
        for d in range(1, size):
            arrive((tag, q, d), incoming.at[rows_at(turn(here, -d, size)), pl.ds(q * cols, cols)])

    def moved(matrix, value):
        return jnp.dot(matrix, value, preferred_element_type=jnp.float32).astype(jnp.bfloat16)

    def span_of(q):
        return slice(q * cols, (q + 1) * cols)

    def d0(q):
        out_z[:, span_of(q)] = moved(place, normed[:, span_of(q)])
        exchange("dz", q, "z", out_z, in_z)

    def d1(q):
        exchanged("dz", q, "z", in_z)
        out_x[:, span_of(q)] = moved(swap, in_z[:, span_of(q)])
        exchange("dx", q, "x", out_x, rows_all.at[y])

    def d2(q):
        exchanged("dx", q, "x", rows_all.at[y])
        spread(("dy", q), rows_all, chunk_of(q))

    def d3(q):
        spread_pass(("dy", q), rows_all, chunk_of(q))

    def d4(q):
        spread_done(("dy", q), rows_all, chunk_of(q))
        x = rows_all[:, :, span_of(q)].reshape(tp * slots, cols)
        if q == 0:
            loads[3].wait()
            loads[4].wait()
        g = jnp.dot(x, wg[span_of(q), :], preferred_element_type=jnp.float32)
        u = jnp.dot(x, wu[span_of(q), :], preferred_element_type=jnp.float32)
        gate[...] = g if q == 0 else gate[...] + g
        up[...] = u if q == 0 else up[...] + u

    def act(g, u):
        return (g / (1.0 + jnp.exp(-g)) * u).astype(jnp.bfloat16)

    def shared_in():
        spread_done("tok", tokens, all_of)
        loads[1].wait()
        loads[2].wait()
        x = tokens[...].reshape(tp * rows, width)
        g = jnp.dot(x, sg[...], preferred_element_type=jnp.float32)
        u = jnp.dot(x, su[...], preferred_element_type=jnp.float32)
        shared_hidden[...] = act(g, u)

    def e0(q):
        p = jnp.dot(hidden[...], wd[:, span_of(q)], preferred_element_type=jnp.float32)
        part[:, :slots, span_of(q)] = p.astype(jnp.bfloat16).reshape(tp, slots, cols)
        s = jnp.dot(shared_hidden[...], sd[:, span_of(q)], preferred_element_type=jnp.float32)
        part[:, slots:, span_of(q)] = s.astype(jnp.bfloat16).reshape(tp, rows, cols)
        sum_far(("ry", q), part, part_far, chunk_of(q))

    def e1(q):
        sum_pass(("ry", q), part, part_far, part_in, chunk_of(q))

    def e2(q):
        acc = sum_done(("ry", q), part, part_in, chunk_of(q)).astype(jnp.bfloat16)
        back_x[:, span_of(q)] = acc[:slots]
        shared_sum[:, span_of(q)] = acc[slots:]
        exchange("rx", q, "x", back_x, in_bx)

    def e3(q):
        exchanged("rx", q, "x", in_bx)
        back_z[:, span_of(q)] = moved(swap, in_bx[:, span_of(q)])
        exchange("rz", q, "z", back_z, in_bz)

    def e4(q):
        exchanged("rz", q, "z", in_bz)
        got = in_bz[:, span_of(q)]
        routed = [
            jnp.dot(pick[k], got, preferred_element_type=jnp.float32) * rw_ref[:, k : k + 1]
            for k in (0, 1)
        ]
        combined = routed[0] + routed[1] + shared_sum[:, span_of(q)].astype(jnp.float32)
        total[:, span_of(q)] = ALPHA * normed[:, span_of(q)].astype(jnp.float32) + combined

    d0(0)
    spread("tok", tokens, all_of)
    for q in range(1, chunks):
        d0(q)

    def pipeline(stages, extra):
        for at in range(chunks + len(stages) - 1):
            for s, stage in enumerate(stages):
                if 0 <= at - s < chunks:
                    stage(at - s)
            if at in extra:
                extra[at]()

    pipeline((d1, d2, d3, d4), {0: lambda: spread_pass("tok", tokens, all_of), 1: shared_in})
    hidden[...] = act(gate[...], up[...])
    loads[5].wait()
    loads[6].wait()
    pipeline((e0, e1, e2, e3, e4), {})
    out_ref[...] = norm(total[...], 1)
    for job in started:
        job.wait_send()


def moe(attended, residual, routing, route_weight, norm_gain, norm_bias, w_out,
        w_exp_gate, w_exp_up, w_exp_down, w_shared_gate, w_shared_up, w_shared_down):
    rows, width = residual.shape
    tp = lax.axis_size("tp")
    sp = lax.axis_size("sp")
    rows_z, _ = cross(sp)
    capacity = 2
    slots = sp * capacity
    ff = w_exp_gate.shape[2]
    bf16, f32 = jnp.bfloat16, jnp.float32
    vmem = pl.BlockSpec(memory_space=pltpu.VMEM)
    hbm = pl.BlockSpec(memory_space=pl.ANY)
    both = slots + rows
    scratch = [
        pltpu.VMEM(w_out.shape, bf16),
        pltpu.VMEM((width, ff), bf16),
        pltpu.VMEM((width, ff), bf16),
        pltpu.VMEM((ff, width), bf16),
        pltpu.VMEM(w_shared_gate.shape, bf16),
        pltpu.VMEM(w_shared_up.shape, bf16),
        pltpu.VMEM(w_shared_down.shape, bf16),
        pltpu.VMEM((tp, rows, width), bf16),
        pltpu.VMEM((2, rows // 2, width), bf16),
        pltpu.VMEM((2, rows, width), bf16),
        pltpu.VMEM((rows, width), bf16),
        pltpu.VMEM((tp, rows, width), bf16),
        pltpu.VMEM((slots, width), bf16),
        pltpu.VMEM((slots, width), bf16),
        pltpu.VMEM((slots, width), bf16),
        pltpu.VMEM((tp, slots, width), bf16),
        pltpu.VMEM((tp * slots, ff), f32),
        pltpu.VMEM((tp * slots, ff), f32),
        pltpu.VMEM((tp * rows, w_shared_gate.shape[1]), bf16),
        pltpu.VMEM((tp * slots, ff), bf16),
        pltpu.VMEM((tp, both, width), bf16),
        pltpu.VMEM((2, both // 2, width), bf16),
        pltpu.VMEM((2, both, width), bf16),
        pltpu.VMEM((slots, width), bf16),
        pltpu.VMEM((slots, width), bf16),
        pltpu.VMEM((slots, width), bf16),
        pltpu.VMEM((slots, width), bf16),
        pltpu.VMEM((rows, width), bf16),
        pltpu.VMEM((rows, width), f32),
        pltpu.SemaphoreType.DMA((192,)),
        pltpu.SemaphoreType.DMA((192,)),
        pltpu.SemaphoreType.DMA((7,)),
    ]
    return pl.pallas_call(
        functools.partial(moe_kernel, rows_z, 4, capacity),
        out_shape=jax.ShapeDtypeStruct((rows, width), bf16),
        in_specs=[vmem] * 6 + [hbm] * 7,
        out_specs=vmem,
        scratch_shapes=scratch,
        compiler_params=pltpu.CompilerParams(
            collective_id=1, has_side_effects=True, vmem_limit_bytes=48 * 1024 * 1024
        ),
        name="moe",
    )(attended, residual, routing, route_weight, norm_gain, norm_bias, w_out,
      w_exp_gate, w_exp_up, w_exp_down, w_shared_gate, w_shared_up, w_shared_down)


def per_device(
    residual,
    query_rows,
    key_rows,
    value_rows,
    head_offset,
    w_out,
    norm_gain,
    norm_bias,
    routing,
    route_weight,
    w_exp_gate,
    w_exp_up,
    w_exp_down,
    w_shared_gate,
    w_shared_up,
    w_shared_down,
):
    attended = attend(head_offset, query_rows, key_rows, value_rows)
    return moe(
        attended, residual, routing, route_weight, norm_gain, norm_bias, w_out,
        w_exp_gate, w_exp_up, w_exp_down, w_shared_gate, w_shared_up, w_shared_down,
    )


def solution(mesh):
    placed = (
        P(("sp", "tp"), None),
        P("sp", "tp"),
        P("sp", "tp"),
        P("sp", "tp"),
        P("tp"),
        P("tp", None),
        P(),
        P(),
        P(("sp", "tp"), None),
        P(("sp", "tp"), None),
        P("sp", None, "tp"),
        P("sp", None, "tp"),
        P("sp", "tp", None),
        P(None, "tp"),
        P(None, "tp"),
        P("tp", None),
    )
    return jax.shard_map(
        per_device, mesh=mesh, in_specs=placed, out_specs=P(("sp", "tp"), None), check_vma=False
    )
```

```python
import functools

import jax
import jax.numpy as jnp
from jax import lax
from jax.experimental import pallas as pl
from jax.experimental.pallas import tpu as pltpu
from jax.sharding import PartitionSpec as P

LOG2E = 1.4426950408889634
ALPHA = 8.0**0.25
LN_EPS = 1e-05


def cross(sp_count):
    rows_x = 4
    return sp_count // (2 * rows_x), rows_x


def layer_kernel(rows_z, rows_x, chunks, capacity,
                 off_ref, q_ref, k_ref, v_ref, res_ref, route_ref, rw_ref, gain_ref, bias_ref,
                 wo_hbm, wg_hbm, wu_hbm, wd_hbm, sg_hbm, su_hbm, sd_hbm,
                 out_ref,
                 keys, values, right, left, carry,
                 wo, wg, wu, wd, sg, su, sd,
                 proj, proj_in, normed, tokens,
                 out_z, in_z, out_x, rows_all, gate, up, shared_hidden, hidden, hidden_in,
                 part, part_far, part_in, back_x, in_bx, back_z, in_bz, total,
                 send, recv, local):
    me = lax.axis_index("sp")
    y = lax.axis_index("tp")
    tp = lax.axis_size("tp")
    group = 2 * rows_x
    z, w = lax.div(me, group), lax.rem(me, group)
    x, c = lax.div(w, 2), lax.rem(w, 2)
    q_rows = q_ref.shape[0]
    heads = off_ref.shape[0]
    dh = k_ref.shape[1]
    reach = rows_z // 2
    block = rows_z * capacity
    rows, width = res_ref.shape
    slots = out_z.shape[0]
    cols = width // chunks
    mesh_ids = pl.DeviceIdType.MESH

    def turn(value, by, size):
        return lax.rem(value + (by + size), size)

    def at(zz, xx, cc):
        return {"sp": (zz * rows_x + xx) * 2 + cc}

    y_side = {1: turn(y, 1, tp), -1: turn(y, -1, tp), 2: turn(y, 2, tp)}
    x_side = {1: turn(x, 1, rows_x), -1: turn(x, -1, rows_x), 2: turn(x, 2, rows_x)}
    to_z = {way: at(turn(z, way, rows_z), x, c) for way in (1, -1)}
    to_x = {way: at(z, x_side[way], c) for way in (1, -1, 2)}
    to_y = {way: {"tp": y_side[way]} for way in (1, -1, 2)}
    partner = at(z, x, 1 - c)
    ways = (1, -1)
    every_way = (2, 1, -1)

    barrier = pltpu.get_barrier_semaphore()
    peers = [{"sp": turn(z, d, rows_z) * group + w} for d in range(1, rows_z)]
    peers += [{"sp": z * group + turn(w, d, group)} for d in range(1, group)]
    peers += [to_y[way] for way in every_way]
    for peer in peers:
        pl.semaphore_signal(barrier, inc=1, device_id=peer, device_id_type=mesh_ids)

    loads = []
    for i, (src, dst) in enumerate((
        (wd_hbm.at[0], wd.at[y]), (wo_hbm, wo), (sg_hbm, sg), (su_hbm, su),
        (wg_hbm.at[0], wg), (wu_hbm.at[0], wu), (sd_hbm, sd),
        (k_ref, keys.at[z, x, c]), (v_ref, values.at[z, x, c]),
    )):
        load = pltpu.make_async_copy(src, dst, local.at[i])
        load.start()
        loads.append(load)

    names = {}
    started = []

    def copy(name, src, dst, target):
        slot = names.setdefault(name, len(names))
        return pltpu.make_async_remote_copy(
            src_ref=src, dst_ref=dst, send_sem=send.at[slot], recv_sem=recv.at[slot],
            device_id=target, device_id_type=mesh_ids,
        )

    def begin(name, src, dst, target):
        job = copy(name, src, dst, target)
        job.start()
        started.append(job)

    def arrive(name, dst):
        copy(name, dst, dst, partner).wait_recv()

    def halves(n):
        return {1: pl.ds(0, n // 2), -1: pl.ds(n // 2, n // 2)}

    def span(q):
        return pl.ds(q * cols, cols)

    def span_of(q):
        return slice(q * cols, (q + 1) * cols)

    pl.semaphore_wait(barrier, len(peers))

    own_k, own_v = keys.at[z, x, c], values.at[z, x, c]
    column = {"own": x, "down": x_side[-1], "up": x_side[1], "far": x_side[2]}
    last_way = {"own": 1, "down": 1, "up": -1, "far": -1}
    v_part = halves(q_rows)

    def slab_of(way, step):
        return turn(z, -way * step, rows_z)

    def slabs_at(step):
        if step == 0:
            return ((0, 0),)
        if step == reach:
            return ((1, step),)
        return ((1, step), (-1, step))

    def send_k(way, step, name):
        if step == reach and last_way[name] != way:
            return
        block_ = keys.at[slab_of(way, step - 1), column[name], c]
        src = k_ref if (step == 1 and name == "own") else block_
        begin(("kz", way, step, name), src, block_, to_z[way])

    def pass_k(step, name):
        if not 1 <= step <= reach:
            return
        for way in ways:
            if step == reach and last_way[name] != way:
                continue
            arrive(("kz", way, step, name), keys.at[slab_of(way, step), column[name], c])
            if step < reach:
                send_k(way, step + 1, name)

    def pass_v(step):
        for way in ways:
            zz = slab_of(way, step)
            if step < reach:
                block_ = values.at[zz, x, c]
                arrive(("vz", way, step), block_)
                piece = block_ if step + 1 < reach else values.at[zz, x, c, v_part[way]]
                begin(("vz", way, step + 1), piece, piece, to_z[way])
                for side in every_way:
                    begin(("vx", way, step, side), block_, block_, to_x[side])
            else:
                arrive(("vz", way, step), values.at[zz, x, c, v_part[way]])
        if step == reach:
            block_ = values.at[slab_of(1, step), x, c]
            for side in every_way:
                begin(("vx", 1, step, side), block_, block_, to_x[side])

    def from_x(tag, buf, zz):
        for side in (1, -1, 2):
            arrive(tag + (side,), buf.at[zz, x_side[2 if side == 2 else -side], c])

    def share(tag, buf, zz):
        begin(tag + ("peer",), buf.at[zz, :, c], buf.at[zz, :, c], partner)

    def shared(tag, buf, zz):
        arrive(tag + ("peer",), buf.at[zz, :, 1 - c])

    for way in every_way:
        begin(("kx", way), k_ref, own_k, to_x[way])
    for way in ways:
        send_k(way, 1, "own")
    for way in ways:
        begin(("vz", way, 1), v_ref, own_v, to_z[way])
    for way in every_way:
        begin(("vx", 0, 0, way), v_ref, own_v, to_x[way])
    for q in range(chunks):
        for way in ways:
            begin(("wd", q, way), wd_hbm.at[0, :, span(q)], wd.at[y, :, span(q)], to_y[way])

    def relay_down(q):
        piece = halves(wd.shape[1])
        for way in ways:
            side = y_side[-way]
            arrive(("wd", q, way), wd.at[side, :, span(q)])
            half = wd.at[side, piece[way], span(q)]
            begin(("wd", q, "far", way), half, half, to_y[way])

    def relayed_down(q):
        piece = halves(wd.shape[1])
        for way in ways:
            arrive(("wd", q, "far", way), wd.at[y_side[2], piece[way], span(q)])

    loads[7].wait()
    loads[8].wait()

    scale2 = dh**-0.5 * LOG2E
    sub = 2 * q_rows
    r_at = lax.broadcasted_iota(jnp.int32, (sub, sub), 0)
    c_at = lax.broadcasted_iota(jnp.int32, (sub, sub), 1)
    after_of = jnp.where(r_at > c_at, 1.0, 0.0).astype(jnp.bfloat16)
    t_in_slab = w * q_rows + lax.broadcasted_iota(jnp.int32, (q_rows, sub), 0)

    def slab(zz, carries, masked):
        stage = []
        for j in reversed(range(rows_x)):
            k = keys[zz, j].reshape(sub, dh)
            v = values[zz, j].reshape(sub, dh)
            mask = None
            if masked:
                mask = j * sub + lax.broadcasted_iota(jnp.int32, (q_rows, sub), 1) < t_in_slab
            for h in range(heads):
                q = q_ref[:, h * dh : (h + 1) * dh]
                s = lax.dot_general(q, k, (((1,), (1,)), ((), ())), preferred_element_type=jnp.float32)
                s = s * scale2 + off_ref[h] * LOG2E
                sp = jnp.maximum(s, 0.0) + jnp.log2(1.0 + jnp.exp2(-jnp.abs(s)))
                own = s - sp
                if masked:
                    sp = jnp.where(mask, sp, 0.0)
                hi = sp.astype(jnp.bfloat16)
                lo = (sp - hi.astype(jnp.float32)).astype(jnp.bfloat16)
                after = jnp.dot(hi, after_of, preferred_element_type=jnp.float32)
                after = after + jnp.dot(lo, after_of, preferred_element_type=jnp.float32)
                stage.append((h, own - after, after[:, :1] + sp[:, :1], v, mask))
        carries = list(carries)
        parts = [None] * heads
        for h, exponent, total_, v, mask in stage:
            weight = jnp.exp2(exponent - carries[h])
            if masked:
                weight = jnp.where(mask, weight, 0.0)
            piece = jnp.dot(weight.astype(jnp.bfloat16), v, preferred_element_type=jnp.float32)
            parts[h] = piece if parts[h] is None else parts[h] + piece
            carries[h] = carries[h] + total_
        return parts, carries

    def head_cols(h):
        return slice(h * dh, (h + 1) * dh)

    def put_carry(carries):
        for h in range(heads):
            carry[h] = jnp.broadcast_to(carries[h], (q_rows, dh))

    no_carry = [jnp.zeros((q_rows, 1), jnp.float32)] * heads

    def own_slab():
        parts, carries = slab(z, no_carry, True)
        for h in range(heads):
            right[:, head_cols(h)] = parts[h]
        put_carry(carries)
        left[...] = jnp.zeros_like(left)

    def right_slab(step):
        @pl.when(z >= step)
        def _():
            parts, carries = slab(z - step, [carry[h][:, :1] for h in range(heads)], False)
            for h in range(heads):
                right[:, head_cols(h)] = right[:, head_cols(h)] + parts[h]
            put_carry(carries)

    def left_slab(step):
        @pl.when(z + step >= rows_z)
        def _():
            parts, totals = slab(z + step - rows_z, no_carry, False)
            for h in range(heads):
                left[:, head_cols(h)] = parts[h] + jnp.exp2(-totals[h]) * left[:, head_cols(h)]

    def attend_slabs(step):
        for way, stp in slabs_at(step):
            shared(("k", way, stp), keys, slab_of(way, stp))
            shared(("v", way, stp), values, slab_of(way, stp))
        if step == 0:
            own_slab()
        else:
            right_slab(step)
            if step < reach:
                left_slab(step)

    for wave in range(1, reach + 2):
        pass_k(wave, "own")
        if wave == 1:
            from_x(("kx",), keys, z)
            for name in ("down", "up", "far"):
                for way in ways:
                    send_k(way, 1, name)
        else:
            for name in ("down", "up", "far"):
                pass_k(wave - 1, name)
        if wave <= reach:
            pass_v(wave)
        for way, stp in slabs_at(wave - 1):
            share(("k", way, stp), keys, slab_of(way, stp))
            from_x(("vx", way, stp), values, slab_of(way, stp))
            share(("v", way, stp), values, slab_of(way, stp))
        if 2 <= wave < chunks + 1:
            relay_down(wave - 2)
        if wave >= 2:
            attend_slabs(wave - 2)
    attend_slabs(reach)

    att = jnp.concatenate(
        [
            (right[:, head_cols(h)] + jnp.exp2(-carry[h]) * left[:, head_cols(h)]).astype(jnp.bfloat16)
            for h in range(heads)
        ],
        axis=1,
    )
    loads[1].wait()
    out_part = jnp.dot(att, wo[...], preferred_element_type=jnp.float32).astype(jnp.bfloat16)
    proj[...] = out_part.reshape(tp, rows, width)
    for way in every_way:
        begin(("proj", way), proj.at[y_side[way]], proj_in.at[y], to_y[way])

    t_row = lax.broadcasted_iota(jnp.int32, (rows, rows), 0)
    t_col = lax.broadcasted_iota(jnp.int32, (rows, rows), 1)
    routes = route_ref[...].astype(jnp.float32)
    e_col = [routes[:, k : k + 1] for k in (0, 1)]
    e_row = [jnp.sum(jnp.where(t_row == t_col, e, 0.0), axis=0, keepdims=True) for e in e_col]

    def same(a, b, keep=None):
        hit = jnp.where(a == b, 1.0, 0.0)
        return hit if keep is None else jnp.where(keep, hit, 0.0)

    rank_col = [
        jnp.sum(same(e_col[0], e_row[0], t_col < t_row), axis=1, keepdims=True),
        jnp.sum(same(e_col[1], e_row[0]) + same(e_col[1], e_row[1], t_col < t_row), axis=1, keepdims=True),
    ]
    rank_row = [
        jnp.sum(same(e_col[0], e_row[0], t_row < t_col), axis=0, keepdims=True),
        jnp.sum(same(e_col[0], e_row[1]) + same(e_col[1], e_row[1], t_row < t_col), axis=0, keepdims=True),
    ]
    slot_col = [e_col[k] * capacity + rank_col[k] for k in (0, 1)]
    slot_row = [e_row[k] * capacity + rank_row[k] for k in (0, 1)]
    s_row = lax.broadcasted_iota(jnp.int32, (slots, rows), 0).astype(jnp.float32)
    place = (same(s_row, slot_row[0]) + same(s_row, slot_row[1])).astype(jnp.bfloat16)
    s_col = lax.broadcasted_iota(jnp.int32, (rows, slots), 1).astype(jnp.float32)
    pick = [same(s_col, slot_col[k]).astype(jnp.bfloat16) for k in (0, 1)]
    i_dst = lax.broadcasted_iota(jnp.int32, (slots, slots), 0)
    i_src = lax.broadcasted_iota(jnp.int32, (slots, slots), 1)
    from_row = lax.div(lax.rem(i_dst, block), capacity) * block + lax.div(i_dst, block) * capacity + lax.rem(i_dst, capacity)
    swap = jnp.where(i_src == from_row, 1.0, 0.0).astype(jnp.bfloat16)

    def norm(summed, n):
        center = summed - jnp.mean(summed, axis=-1, keepdims=True)
        spread_ = jnp.mean(center * center, axis=-1, keepdims=True)
        scaled = center * lax.rsqrt(spread_ + LN_EPS) * gain_ref[n : n + 1, :] + bias_ref[n : n + 1, :]
        return scaled.astype(jnp.bfloat16)

    mixed = proj[y].astype(jnp.float32)
    for way in (1, -1, 2):
        source = y_side[2 if way == 2 else -way]
        arrive(("proj", way), proj_in.at[source])
        mixed = mixed + proj_in[source].astype(jnp.float32)
    normed[...] = norm(ALPHA * res_ref[...].astype(jnp.float32) + mixed, 0)
    tokens[y] = normed[...]

    def rows_at(n):
        return pl.ds(pl.multiple_of(n * block, block), block)

    def exchange(tag, q, axis, outgoing, incoming):
        here, size = (z, rows_z) if axis == "z" else (w, group)
        for d in range(1, size):
            there = turn(here, d, size)
            target = {"sp": there * group + w} if axis == "z" else {"sp": z * group + there}
            begin((tag, q, d), outgoing.at[rows_at(there), span(q)], incoming.at[rows_at(here), span(q)], target)
        incoming[rows_at(here), span(q)] = outgoing[rows_at(here), span(q)]

    def exchanged(tag, q, axis, incoming):
        here, size = (z, rows_z) if axis == "z" else (w, group)
        for d in range(1, size):
            arrive((tag, q, d), incoming.at[rows_at(turn(here, -d, size)), span(q)])

    def moved(matrix, value):
        return jnp.dot(matrix, value, preferred_element_type=jnp.float32).astype(jnp.bfloat16)

    def act(g, u):
        return (g / (1.0 + jnp.exp(-g)) * u).astype(jnp.bfloat16)

    def d0(q):
        out_z[:, span_of(q)] = moved(place, normed[:, span_of(q)])
        exchange("dz", q, "z", out_z, in_z)

    def d1(q):
        exchanged("dz", q, "z", in_z)
        out_x[:, span_of(q)] = moved(swap, in_z[:, span_of(q)])
        exchange("dx", q, "x", out_x, rows_all.at[y])

    def d2(q):
        exchanged("dx", q, "x", rows_all.at[y])
        for way in ways:
            begin(("dy", q, way), rows_all.at[y, :, span(q)], rows_all.at[y, :, span(q)], to_y[way])

    row_half = halves(slots)

    def d3(q):
        for way in ways:
            side = y_side[-way]
            arrive(("dy", q, way), rows_all.at[side, :, span(q)])
            half = rows_all.at[side, row_half[way], span(q)]
            begin(("dy", q, "far", way), half, half, to_y[way])

    def d4(q):
        for way in ways:
            arrive(("dy", q, "far", way), rows_all.at[y_side[2], row_half[way], span(q)])
        xs = rows_all[:, :, span_of(q)].reshape(tp * slots, cols)
        if q == 0:
            loads[4].wait()
            loads[5].wait()
        g = jnp.dot(xs, wg[span_of(q), :], preferred_element_type=jnp.float32)
        u = jnp.dot(xs, wu[span_of(q), :], preferred_element_type=jnp.float32)
        gate[...] = g if q == 0 else gate[...] + g
        up[...] = u if q == 0 else up[...] + u

    def shared_in():
        for way in (1, -1, 2):
            arrive(("tok", way), tokens.at[y_side[2 if way == 2 else -way]])
        loads[2].wait()
        loads[3].wait()
        loads[6].wait()
        xs = tokens[...].reshape(tp * rows, width)
        g = jnp.dot(xs, sg[...], preferred_element_type=jnp.float32)
        u = jnp.dot(xs, su[...], preferred_element_type=jnp.float32)
        shared_hidden[...] = act(g, u)
        s = jnp.dot(shared_hidden[...], sd[...], preferred_element_type=jnp.float32)
        part[...] = s.astype(jnp.bfloat16).reshape(tp, rows, width)

    piece = halves(rows)

    def shared_far():
        for way in ways:
            begin(("sh", "far", way), part.at[y_side[2], piece[way]], part_far.at[0 if way == 1 else 1], to_y[way])

    def shared_pass():
        for way in ways:
            n = 0 if way == 1 else 1
            arrive(("sh", "far", way), part_far.at[n])
            mine = part.at[y_side[way], piece[way]]
            mine[...] = (mine[...].astype(jnp.float32) + part_far[n].astype(jnp.float32)).astype(jnp.bfloat16)
            begin(("sh", "near", way), part.at[y_side[way]], part_in.at[n], to_y[way])

    def shared_out():
        acc = part[y].astype(jnp.float32)
        for way in ways:
            n = 0 if way == 1 else 1
            arrive(("sh", "near", way), part_in.at[n])
            acc = acc + part_in[n].astype(jnp.float32)
        total[...] = ALPHA * normed[...].astype(jnp.float32) + acc.astype(jnp.bfloat16).astype(jnp.float32)

    def e0(q):
        acc = jnp.dot(hidden_in[0], wd[0, :, span_of(q)], preferred_element_type=jnp.float32)
        for j in range(1, tp):
            acc = acc + jnp.dot(hidden_in[j], wd[j, :, span_of(q)], preferred_element_type=jnp.float32)
        back_x[:, span_of(q)] = acc.astype(jnp.bfloat16)
        exchange("rx", q, "x", back_x, in_bx)

    def e1(q):
        exchanged("rx", q, "x", in_bx)
        back_z[:, span_of(q)] = moved(swap, in_bx[:, span_of(q)])
        exchange("rz", q, "z", back_z, in_bz)

    def e2(q):
        exchanged("rz", q, "z", in_bz)
        got = in_bz[:, span_of(q)]
        routed = [
            jnp.dot(pick[k], got, preferred_element_type=jnp.float32) * rw_ref[:, k : k + 1]
            for k in (0, 1)
        ]
        total[:, span_of(q)] = total[:, span_of(q)] + (routed[0] + routed[1])

    d0(0)
    for way in every_way:
        begin(("tok", way), tokens.at[y], tokens.at[y], to_y[way])
    for q in range(1, chunks):
        d0(q)

    def pipeline(stages, extra):
        for step in range(chunks + len(stages) - 1):
            for s, stage in enumerate(stages):
                if 0 <= step - s < chunks:
                    stage(step - s)
            if step in extra:
                extra[step]()

    pipeline((d1, d2, d3, d4), {0: shared_in, chunks: shared_far, chunks + 1: lambda: relay_down(chunks - 1)})
    hidden[...] = act(gate[...], up[...]).reshape(tp, slots, hidden.shape[2])
    for way in every_way:
        begin(("hid", way), hidden.at[y_side[way]], hidden_in.at[y], to_y[way])
    hidden_in[y] = hidden[y]
    shared_pass()
    loads[0].wait()
    for q in range(chunks):
        relayed_down(q)
    for way in (1, -1, 2):
        arrive(("hid", way), hidden_in.at[y_side[2 if way == 2 else -way]])
    pipeline((e0, e1, e2), {0: shared_out})
    out_ref[...] = norm(total[...], 1)
    for job in started:
        job.wait_send()


def layer(head_offset, query_rows, key_rows, value_rows, residual, routing, route_weight,
          norm_gain, norm_bias, w_out, w_exp_gate, w_exp_up, w_exp_down,
          w_shared_gate, w_shared_up, w_shared_down):
    rows, width = residual.shape
    q_rows, q_width = query_rows.shape
    dh = key_rows.shape[1]
    heads = head_offset.shape[0]
    tp = lax.axis_size("tp")
    sp = lax.axis_size("sp")
    rows_z, rows_x = cross(sp)
    capacity = 2
    slots = sp * capacity
    ff = w_exp_gate.shape[2]
    bf16, f32 = jnp.bfloat16, jnp.float32
    vmem = pl.BlockSpec(memory_space=pltpu.VMEM)
    hbm = pl.BlockSpec(memory_space=pl.ANY)
    kv = pltpu.VMEM((rows_z, rows_x, 2, q_rows, dh), bf16)
    routed = pltpu.VMEM((slots, width), bf16)
    scratch = [
        kv,
        kv,
        pltpu.VMEM((q_rows, q_width), f32),
        pltpu.VMEM((q_rows, q_width), f32),
        pltpu.VMEM((heads, q_rows, dh), f32),
        pltpu.VMEM(w_out.shape, bf16),
        pltpu.VMEM((width, ff), bf16),
        pltpu.VMEM((width, ff), bf16),
        pltpu.VMEM((tp, ff, width), bf16),
        pltpu.VMEM(w_shared_gate.shape, bf16),
        pltpu.VMEM(w_shared_up.shape, bf16),
        pltpu.VMEM(w_shared_down.shape, bf16),
        pltpu.VMEM((tp, rows, width), bf16),
        pltpu.VMEM((tp, rows, width), bf16),
        pltpu.VMEM((rows, width), bf16),
        pltpu.VMEM((tp, rows, width), bf16),
        routed,
        routed,
        routed,
        pltpu.VMEM((tp, slots, width), bf16),
        pltpu.VMEM((tp * slots, ff), f32),
        pltpu.VMEM((tp * slots, ff), f32),
        pltpu.VMEM((tp * rows, w_shared_gate.shape[1]), bf16),
        pltpu.VMEM((tp, slots, ff), bf16),
        pltpu.VMEM((tp, slots, ff), bf16),
        pltpu.VMEM((tp, rows, width), bf16),
        pltpu.VMEM((2, rows // 2, width), bf16),
        pltpu.VMEM((2, rows, width), bf16),
        routed,
        routed,
        routed,
        routed,
        pltpu.VMEM((rows, width), f32),
        pltpu.SemaphoreType.DMA((288,)),
        pltpu.SemaphoreType.DMA((288,)),
        pltpu.SemaphoreType.DMA((9,)),
    ]
    return pl.pallas_call(
        functools.partial(layer_kernel, rows_z, rows_x, 4, capacity),
        out_shape=jax.ShapeDtypeStruct((rows, width), bf16),
        in_specs=[pl.BlockSpec(memory_space=pltpu.SMEM)] + [vmem] * 8 + [hbm] * 7,
        out_specs=vmem,
        scratch_shapes=scratch,
        compiler_params=pltpu.CompilerParams(
            collective_id=0, has_side_effects=True, vmem_limit_bytes=67043328
        ),
        name="layer",
    )(head_offset, query_rows, key_rows, value_rows, residual, routing, route_weight,
      norm_gain, norm_bias, w_out, w_exp_gate, w_exp_up, w_exp_down,
      w_shared_gate, w_shared_up, w_shared_down)


def per_device(
    residual,
    query_rows,
    key_rows,
    value_rows,
    head_offset,
    w_out,
    norm_gain,
    norm_bias,
    routing,
    route_weight,
    w_exp_gate,
    w_exp_up,
    w_exp_down,
    w_shared_gate,
    w_shared_up,
    w_shared_down,
):
    return layer(
        head_offset, query_rows, key_rows, value_rows, residual, routing, route_weight,
        norm_gain, norm_bias, w_out, w_exp_gate, w_exp_up, w_exp_down,
        w_shared_gate, w_shared_up, w_shared_down,
    )


def solution(mesh):
    placed = (
        P(("sp", "tp"), None),
        P("sp", "tp"),
        P("sp", "tp"),
        P("sp", "tp"),
        P("tp"),
        P("tp", None),
        P(),
        P(),
        P(("sp", "tp"), None),
        P(("sp", "tp"), None),
        P("sp", None, "tp"),
        P("sp", None, "tp"),
        P("sp", "tp", None),
        P(None, "tp"),
        P(None, "tp"),
        P("tp", None),
    )
    return jax.shard_map(
        per_device, mesh=mesh, in_specs=placed, out_specs=P(("sp", "tp"), None), check_vma=False
    )
```
